512 devices in a mesh: sp: 64 (over z, y), tp: 4 (over x), dp: 2 (over core).
Axes of the slice: x: 4, y: 8, z: 8, core: 2. Of those that a mesh axis runs over, the one named last changes fastest.
Arguments:
- latent: bfloat16 [2, 16384, 2048], P('dp', ('sp', 'tp')), may hold values from -6 to 6
- condition: bfloat16 [2, 2048], P('dp', ('sp', 'tp')), may hold values from -6 to 6
- context: bfloat16 [2, 512, 2048], P('dp', 'sp'), may hold values from -6 to 6
- context_vector: bfloat16 [2048], P(('sp', 'tp')), may hold values from -6 to 6
- modulator: bfloat16 [2048, 6144], P(('sp', 'tp')), may hold values from -0.3125 to 0.3125
- norm_gain: float32 [2048], replicated, may hold values from 0.1 to 1.9
- query_weight: bfloat16 [2048, 512], P(None, 'tp'), may hold values from -4 to 4
- key_weight: bfloat16 [2048, 512], P(None, 'tp'), may hold values from -0.125 to 0.125
- value_weight: bfloat16 [2048, 512], P(None, 'tp'), may hold values from -0.125 to 0.125
- head_gain: float32 [128], replicated, may hold values from 0.1 to 1.9
- lambdas: float32 [4], P('tp'), may hold values from 0.3 to 0.8
- context_bias: float32 [4, 2], P('tp'), may hold values from 1.3 to 2.7
- out_weight: bfloat16 [512, 2048], P('tp'), may hold values from -0.25 to 0.25
Outputs:
- updated: bfloat16 [2, 16384, 2048], P('dp', ('sp', 'tp'))
The draws below stay inside these ranges and needn't reach their ends.
All inputs are finite; a program needn't handle non-finite values.
Results may differ from the reference program's by a relative error of at most 0.024.
Values may be sent and summed in bfloat16 or wider, within the bound.
A program may use at most 64 MiB of HBM per device.

```python
import math
import jax
import jax.numpy as jnp
from jax import lax

D = 2048
HEADS = 4
HEAD = 64
SEQ = 16384
CTX = 512
SAMPLES = 2


def query_key_pair(key):
    key_spread = (1.5 * D) ** (-0.5)
    query_spread = (3.0 * D) ** (-0.5)
    key_part = key_spread * jax.random.normal(jax.random.fold_in(key, 11), (D, HEADS, 2, HEAD), jnp.float32)
    key_part = jnp.clip(key_part, -0.12, 0.12)
    query_part = query_spread * jax.random.normal(jax.random.fold_in(key, 12), (D, HEADS, 2, HEAD), jnp.float32)
    query_part = jnp.clip(query_part, -4.0, 4.0)
    return (query_part.reshape(D, HEADS * 2 * HEAD), key_part.reshape(D, HEADS * 2 * HEAD))


def draw_query_weight(key, part):
    return query_key_pair(key)[0].astype(jnp.bfloat16)


def draw_key_weight(key, part):
    return query_key_pair(key)[1].astype(jnp.bfloat16)


def steps_of(rng, extent, split, least, high):
    def one(dim, parts):
        heights = jax.random.uniform(jax.random.fold_in(jax.random.fold_in(rng, 6), dim), (parts,), jnp.float32, least / len(split), high / len(split))
        return jnp.repeat(jnp.exp(heights), extent[dim] // parts).reshape((-1,) + (1,) * (len(extent) - dim - 1))

    level = one(*split[0])
    for cut in split[1:]:
        level = level * one(*cut)
    return level


def noise(stream_key, dims, width, reach, shards=(), kind=jnp.bfloat16):
    result = jax.random.normal(stream_key, dims, jnp.float32) * width
    if len(shards) > 0:
        result = steps_of(stream_key, dims, shards, -0.22, 0.18) * result
    return jnp.clip(result, min=-reach, max=reach).astype(kind)


def setup_inputs(seed: int = 0) -> dict:
    key_of = jax.random.split(jax.random.key(seed), 14)
    return {
        "latent": noise(key_of[0], (SAMPLES, SEQ, D), 1.0, 6.0, ((0, 2), (1, 256))),
        "condition": noise(key_of[1], (SAMPLES, D), 1.0, 6.0, ((0, 2), (1, 256))),
        "context": noise(key_of[2], (SAMPLES, CTX, D), 1.0, 6.0, ((0, 2), (1, 64))),
        "context_vector": noise(key_of[3], (D,), 1.0, 6.0, ((0, 256),)),
        "modulator": noise(key_of[4], (D, 3 * D), (D // 6) ** -0.5, 0.3125, ((0, 256),)),
        "norm_gain": jnp.clip(1.0 + 0.18 * jax.random.normal(key_of[5], (D,), jnp.float32), 0.1, 1.9),
        "query_weight": draw_query_weight(jax.random.fold_in(key_of[13], 71), 0),
        "key_weight": draw_key_weight(jax.random.fold_in(key_of[13], 71), 0),
        "value_weight": noise(key_of[8], (D, 2 * HEAD * HEADS), D ** -0.5, 0.125, ((1, 4),)),
        "head_gain": jnp.clip(1.0 + 0.18 * jax.random.normal(key_of[9], (2 * HEAD,), jnp.float32), 0.1, 1.9),
        "lambdas": jnp.clip(0.3 + 0.5 * jax.random.uniform(key_of[10], (HEADS,), jnp.float32) ** steps_of(key_of[10], (HEADS,), ((0, 4),), -0.2, 0.2), 0.3, 0.8),
        "context_bias": jnp.clip(1.3 + 1.4000001 * jax.random.uniform(key_of[11], (HEADS, 2), jnp.float32) ** steps_of(key_of[11], (HEADS, 2), ((0, 4),), -0.2, 0.2), 1.3, 2.7),
        "out_weight": noise(key_of[12], (2 * HEAD * HEADS, D), (2 * HEAD * HEADS) ** -0.5, 0.25, ((0, 4),)),
    }


EPSILON = 1e-06
OUT_SCALE = 0.8

def modulate(inputs, gain_vector, shift_vector, scale_vector):
    as_float = inputs.astype(jnp.float32)
    normed = as_float * lax.rsqrt(lax.optimization_barrier(jnp.mean(as_float * as_float, axis=-1, keepdims=True)) + EPSILON)
    return (normed * gain_vector * (1.0 + scale_vector) + shift_vector).astype(jnp.bfloat16)

def reference(latent, condition, context, context_vector, modulator, norm_gain, query_weight, key_weight, value_weight, head_gain, lambdas, context_bias, out_weight):
    activated = jax.nn.silu(jnp.concatenate([condition, context_vector[None, :]], axis=0).astype(jnp.float32))
    activated = activated.astype(jnp.bfloat16)
    modulations = jnp.dot(activated, modulator, preferred_element_type=jnp.float32)
    ctx_shift = modulations[SAMPLES, :D]
    ctx_scale = modulations[SAMPLES, D:2 * D]
    block_rows = math.gcd(SEQ, 512)
    key_flags = jnp.concatenate([jnp.zeros((SEQ,), jnp.float32), jnp.ones((CTX,), jnp.float32)])
    key_bias = context_bias[:, :, None, None] * key_flags
    results = []
    for sample_index in range(SAMPLES):
        shift_vector = modulations[sample_index, :D]
        scale_vector = modulations[sample_index, D:2 * D]
        gate_vector = modulations[sample_index, 2 * D:]
        hidden = modulate(latent[sample_index], norm_gain, shift_vector, scale_vector)
        ctx_hidden = modulate(context[sample_index], norm_gain, ctx_shift, ctx_scale)
        queries = jnp.dot(hidden, query_weight, preferred_element_type=jnp.float32).astype(jnp.bfloat16)
        queries = queries.reshape(SEQ, HEADS, 2, HEAD)
        all_keys = jnp.concatenate([jnp.dot(hidden, key_weight, preferred_element_type=jnp.float32).astype(jnp.bfloat16), jnp.dot(ctx_hidden, key_weight, preferred_element_type=jnp.float32).astype(jnp.bfloat16)], axis=0)
        all_values = jnp.concatenate([jnp.dot(hidden, value_weight, preferred_element_type=jnp.float32).astype(jnp.bfloat16), jnp.dot(ctx_hidden, value_weight, preferred_element_type=jnp.float32).astype(jnp.bfloat16)], axis=0)
        keys_float = all_keys.reshape(SEQ + CTX, HEADS, 2, HEAD).astype(jnp.float32)
        values_float = all_values.reshape(SEQ + CTX, HEADS, 2 * HEAD).astype(jnp.float32)

        def attend(query_block):
            scores = jnp.einsum('qhmd,khmd->hmqk', query_block.astype(jnp.float32), keys_float) * HEAD ** (-0.5)
            scores = scores + key_bias
            row_max = lax.optimization_barrier(jnp.max(scores, axis=-1, keepdims=True))
            weights = jnp.exp(scores - row_max)
            totals = lax.optimization_barrier(jnp.sum(weights, axis=-1))
            rounded = lax.optimization_barrier(weights.astype(jnp.bfloat16)).astype(jnp.float32)
            summed = jnp.einsum('hmqk,khe->hmqe', rounded, values_float)
            mixed = summed[:, 0] / totals[:, 0, :, None] - lambdas[:, None, None] * summed[:, 1] / totals[:, 1, :, None]
            normed = mixed * lax.rsqrt(lax.optimization_barrier(jnp.mean(mixed * mixed, axis=-1, keepdims=True)) + EPSILON) * head_gain * OUT_SCALE
            return jnp.transpose(normed, (1, 0, 2)).reshape(block_rows, HEADS * 2 * HEAD).astype(jnp.bfloat16)
        query_blocks = queries.reshape(SEQ // block_rows, block_rows, HEADS, 2, HEAD)
        attended = lax.map(attend, query_blocks).reshape(SEQ, HEADS * 2 * HEAD)
        branch = jnp.dot(attended, out_weight, preferred_element_type=jnp.float32)
        results.append((latent[sample_index].astype(jnp.float32) + gate_vector * branch).astype(jnp.bfloat16))
    return jnp.stack(results)
```

```python
import jax
import jax.numpy as jnp
from jax import lax
from jax.experimental import pallas as pl
from jax.experimental.pallas import tpu as pltpu
from jax.sharding import Mesh
from jax.sharding import PartitionSpec as P

SP_TP = ("sp_0", "sp_1", "tp")
SP = ("sp_0", "sp_1")
AXES = ("sp_1", "sp_0")

EPSILON = 1e-06
OUT_SCALE = 0.8
LOG2E = 1.4426950408889634

D = 2048
HEAD = 64
VAL = 128
ROWS = 64
NX = 4
NR = 8
BLOCK = ROWS * NX
CTX = 8
TALL = BLOCK + 2 * CTX
CHUNK = 3 * D // NX
MESH_ID = pl.DeviceIdType.MESH
NT = (((1,), (1,)), ((), ()))
F32 = jnp.float32
BF16 = jnp.bfloat16


def dot(a, b):
    return jnp.dot(a, b, preferred_element_type=F32)


def slot_left(d):
    return 8 - 2 * d


def slot_right(d):
    return 7 - 2 * d


def kernel(
    latent,
    condition,
    context,
    context_vector,
    modulator,
    norm_gain,
    query_weight,
    key_weight,
    value_weight,
    head_gain,
    lambdas,
    context_bias,
    out_weight,
    out,
    mod_v,
    part,
    xrs,
    ysum,
    zsum,
    xag,
    lat,
    ctx_v,
    gain_v,
    hgain_v,
    w_v,
    ow,
    normed_v,
    hidden_v,
    gx,
    gv,
    kctx,
    vctx,
    s_v,
    so,
    sl,
    ro,
    rl,
    att,
    attr,
    res,
    local_sem,
    mod_send,
    mod_recv,
    lat_send,
    lat_recv,
    ow_send,
    ow_recv,
    ring_send,
    ring_recv,
    o_send,
    o_recv,
    l_send,
    l_recv,
    a_send,
    a_recv,
):
    z = lax.axis_index("sp_0")
    y = lax.axis_index("sp_1")
    x = lax.axis_index("tp")
    place = (y, z)

    def remote(src, dst, send, recv, axis, target):
        return pltpu.make_async_remote_copy(
            src_ref=src,
            dst_ref=dst,
            send_sem=send,
            recv_sem=recv,
            device_id={axis: target},
            device_id_type=MESH_ID,
        )

    barrier = pltpu.get_barrier_semaphore()
    for d in range(1, NX):
        pl.semaphore_signal(
            barrier, inc=1, device_id={"tp": lax.rem(x + d, NX)}, device_id_type=MESH_ID
        )
    for axis, here in zip(AXES, place):
        for d in range(1, NR):
            pl.semaphore_signal(
                barrier, inc=1, device_id={axis: lax.rem(here + d, NR)}, device_id_type=MESH_ID
            )

    loads = {
        "mod": pltpu.make_async_copy(modulator, mod_v, local_sem.at[0]),
        "lat": pltpu.make_async_copy(latent.at[0], lat.at[x], local_sem.at[1]),
        "ctx": pltpu.make_async_copy(context.at[0], ctx_v, local_sem.at[2]),
        "gain": pltpu.make_async_copy(norm_gain, gain_v, local_sem.at[3]),
        "hgain": pltpu.make_async_copy(head_gain, hgain_v, local_sem.at[4]),
        "q": pltpu.make_async_copy(query_weight, w_v.at[:, pl.ds(0, VAL)], local_sem.at[5]),
        "k": pltpu.make_async_copy(key_weight, w_v.at[:, pl.ds(VAL, VAL)], local_sem.at[6]),
        "v": pltpu.make_async_copy(value_weight, w_v.at[:, pl.ds(2 * VAL, VAL)], local_sem.at[7]),
        "ow": pltpu.make_async_copy(out_weight, ow.at[x], local_sem.at[8]),
    }
    for name in loads:
        loads[name].start()

    loads["mod"].wait()
    vectors = jnp.concatenate(
        [condition[...].astype(F32), context_vector[...].astype(F32)], axis=0
    )
    activated = (vectors / (1.0 + jnp.exp(-vectors))).astype(BF16).astype(F32)
    for c in range(NX):
        terms = dot(activated, mod_v[:, c * CHUNK : (c + 1) * CHUNK].astype(F32))
        part[c] = terms
    xrs[x] = part[x]
    loads["lat"].wait()

    pl.semaphore_wait(barrier, NX - 1 + 2 * (NR - 1))

    first = []
    for d in range(1, NX):
        to = lax.rem(x + d, NX)
        first.append(remote(part.at[to], xrs.at[x], mod_send.at[d], mod_recv.at[d], "tp", to))
    for copy in first:
        copy.start()

    right, left = lax.rem(x + 1, NX), lax.rem(x + NX - 1, NX)
    far = lax.rem(x + 2, NX)
    half = ROWS // 2
    lat_right = remote(lat.at[x], lat.at[x], lat_send.at[0], lat_recv.at[0], "tp", right)
    lat_left = remote(lat.at[x], lat.at[x], lat_send.at[1], lat_recv.at[1], "tp", left)
    lat_right.start()
    lat_left.start()

    for copy in first:
        copy.wait()
    ysum[y] = xrs[0] + xrs[1] + xrs[2] + xrs[3]

    second = []
    for d in range(1, NR):
        to = lax.rem(y + d, NR)
        second.append(
            remote(ysum.at[y], ysum.at[y], mod_send.at[8 + d], mod_recv.at[8 + d], "sp_1", to)
        )
    for copy in second:
        copy.start()
    for copy in second:
        copy.wait()
    zsum[z] = jnp.sum(ysum[...], axis=0)
    third = []
    for d in range(1, NR):
        to = lax.rem(z + d, NR)
        third.append(
            remote(zsum.at[z], zsum.at[z], mod_send.at[16 + d], mod_recv.at[16 + d], "sp_0", to)
        )
    for copy in third:
        copy.start()

    lat_right.wait()
    relay_right = remote(
        lat.at[left, pl.ds(0, half)],
        lat.at[left, pl.ds(0, half)],
        lat_send.at[2],
        lat_recv.at[2],
        "tp",
        right,
    )
    relay_right.start()
    lat_left.wait()
    relay_left = remote(
        lat.at[right, pl.ds(half, half)],
        lat.at[right, pl.ds(half, half)],
        lat_send.at[3],
        lat_recv.at[3],
        "tp",
        left,
    )
    relay_left.start()

    def normalise(rows):
        as_float = rows.astype(F32)
        return as_float * lax.rsqrt(
            jnp.mean(as_float * as_float, axis=-1, keepdims=True) + EPSILON
        )

    def normalise_block(b):
        base = pl.multiple_of(b * ROWS, ROWS)
        normed_v[pl.ds(base, ROWS), :] = normalise(lat[b])

    normalise_block(x)
    normalise_block(left)
    normalise_block(right)
    loads["ctx"].wait()
    normed_v[pl.ds(BLOCK, CTX), :] = normalise(ctx_v[...])

    for copy in third:
        copy.wait()
    xag[x] = jnp.sum(zsum[...], axis=0)
    fourth = []
    for d in range(1, NX):
        to = lax.rem(x + d, NX)
        fourth.append(
            remote(xag.at[x], xag.at[x], mod_send.at[24 + d], mod_recv.at[24 + d], "tp", to)
        )
    for copy in fourth:
        copy.start()

    loads["ow"].wait()
    ow_right = remote(ow.at[x], ow.at[x], ow_send.at[0], ow_recv.at[0], "tp", right)
    ow_left = remote(ow.at[x], ow.at[x], ow_send.at[1], ow_recv.at[1], "tp", left)
    ow_right.start()
    ow_left.start()

    relay_right.wait()
    relay_left.wait()
    normalise_block(far)
    for name in ("gain", "q", "k", "v", "hgain"):
        loads[name].wait()
    for copy in fourth:
        copy.wait()

    def modulation(row, first_lane):
        pieces = []
        at = first_lane
        while at < first_lane + D:
            c = at // CHUNK
            stop = min(first_lane + D, (c + 1) * CHUNK)
            pieces.append(xag[c, row : row + 1, at - c * CHUNK : stop - c * CHUNK])
            at = stop
        return jnp.concatenate(pieces, axis=1)

    gain = gain_v[...]
    multiplier = gain * (1.0 + modulation(0, D))
    shift = modulation(0, 0)

    for b in range(NX):
        rows = slice(b * ROWS, (b + 1) * ROWS)
        hidden_v[rows, :] = (normed_v[rows, :] * multiplier + shift).astype(BF16)
    ctx_hidden = normed_v[BLOCK : BLOCK + CTX, :] * (
        gain * (1.0 + modulation(1, D))
    ) + modulation(1, 0)
    hidden_v[BLOCK:TALL, :] = jnp.concatenate(
        [ctx_hidden, jnp.zeros_like(ctx_hidden)], axis=0
    ).astype(BF16)

    projected = dot(hidden_v[...], w_v[...])
    q = projected[:BLOCK, :VAL] * (HEAD ** (-0.5) * LOG2E)
    k = projected[:BLOCK, VAL : 2 * VAL]
    v = projected[:BLOCK, 2 * VAL :]
    low = lax.broadcasted_iota(jnp.int32, (BLOCK, VAL), 1) < HEAD
    own = NR - 1
    tail = jnp.concatenate(
        [projected[BLOCK : BLOCK + CTX, VAL : 2 * VAL], projected[BLOCK : BLOCK + CTX, 2 * VAL :]],
        axis=0,
    )
    gx[0, own] = jnp.concatenate([jnp.where(low, k, q), tail], axis=0).astype(BF16)
    gx[1, own] = jnp.concatenate([jnp.where(low, q, k), tail], axis=0).astype(BF16)
    transposed = jnp.transpose(v).astype(BF16)
    gv[0, own] = transposed
    gv[1, own] = transposed

    def ring_copies(a, step):
        axis, here = AXES[a], place[a]
        to_right, to_left = lax.rem(here + 1, NR), lax.rem(here + NR - 1, NR)
        from_left = own if step == 0 else slot_left(step)
        from_right = own if step == 0 else slot_right(step)
        last = step == NR // 2 - 1
        copies = []
        for part_index, buffer in ((0, gx), (1, gv)):
            if not (last and part_index == 1):
                at = ((a * 2) * 4 + step) * 2 + part_index
                copies.append(
                    remote(
                        buffer.at[a, from_left],
                        buffer.at[a, slot_left(step + 1)],
                        ring_send.at[at],
                        ring_recv.at[at],
                        axis,
                        to_right,
                    )
                )
            if not (last and part_index == 0):
                at = ((a * 2 + 1) * 4 + step) * 2 + part_index
                copies.append(
                    remote(
                        buffer.at[a, from_right],
                        buffer.at[a, slot_left(NR // 2) if last else slot_right(step + 1)],
                        ring_send.at[at],
                        ring_recv.at[at],
                        axis,
                        to_left,
                    )
                )
        return copies

    rings = [[ring_copies(a, step) for step in range(4)] for a in range(2)]
    for a in range(2):
        for copy in rings[a][0]:
            copy.start()
    for step in range(1, 4):
        for index in range(4):
            for a in range(2):
                rings[a][step - 1][index].wait_recv()
                if step < 3:
                    rings[a][step][index].start()
                elif index == 0:
                    rings[a][3][0].start()
                elif index == 3:
                    rings[a][3][1].start()
    for a in range(2):
        for copy in rings[a][3]:
            copy.wait_recv()

    ow_right.wait()
    ow_left.wait()
    ow_half = VAL // 2
    ow_relay_right = remote(
        ow.at[left, pl.ds(0, ow_half)],
        ow.at[left, pl.ds(0, ow_half)],
        ow_send.at[2],
        ow_recv.at[2],
        "tp",
        right,
    )
    ow_relay_left = remote(
        ow.at[right, pl.ds(ow_half, ow_half)],
        ow.at[right, pl.ds(ow_half, ow_half)],
        ow_send.at[3],
        ow_recv.at[3],
        "tp",
        left,
    )
    ow_relay_right.start()
    ow_relay_left.start()

    for a in range(2):
        tails = [gx[a, j, BLOCK:TALL, :].astype(F32) for j in range(NR)]
        kctx[a] = jnp.concatenate([t[:CTX] for t in tails], axis=0).astype(BF16)
        rows = jnp.concatenate(
            [t[CTX:] for t in tails] + [jnp.zeros((VAL - NR * CTX, VAL), F32)], axis=0
        )
        vctx[a] = jnp.transpose(rows)[:, : NR * CTX].astype(BF16)

    lane = lax.broadcasted_iota(jnp.int32, (1, VAL), 1)
    is_low = jnp.where(lane < HEAD, 1.0, 0.0)
    masks = (is_low.astype(BF16), (1.0 - is_low).astype(BF16))

    def first_pass(a, t):
        masked = gx[1 - a, t, 0:BLOCK, :] * masks[a]
        top = None
        for j in range(NR):
            scores = lax.dot_general(
                gx[a, j, 0:BLOCK, :], masked, NT, preferred_element_type=F32
            )
            s_v[a, j * BLOCK : (j + 1) * BLOCK, :] = scores
            block_top = jnp.max(scores.reshape(BLOCK // 8, 8, BLOCK), axis=0)
            top = block_top if top is None else jnp.maximum(top, block_top)
            yield None
        ctx_scores = (
            lax.dot_general(kctx[a], masked, NT, preferred_element_type=F32)
            + context_bias[0, a] * LOG2E
        )
        top = jnp.maximum(top, jnp.max(ctx_scores.reshape(NR * CTX // 8, 8, BLOCK), axis=0))
        top = jnp.broadcast_to(jnp.max(top, axis=0, keepdims=True), (8, BLOCK))
        yield (top, ctx_scores)

    def second_pass(a, t, top, ctx_scores):
        weights = jnp.exp2(ctx_scores.reshape(NR * CTX // 8, 8, BLOCK) - top[None])
        total = jnp.sum(weights, axis=0)
        acc = dot(vctx[a], weights.reshape(NR * CTX, BLOCK).astype(BF16))
        for j in range(NR):
            scores = s_v[a, j * BLOCK : (j + 1) * BLOCK, :]
            weights = jnp.exp2(scores.reshape(BLOCK // 8, 8, BLOCK) - top[None])
            total = total + jnp.sum(weights, axis=0)
            acc = acc + dot(gv[a, j], weights.reshape(BLOCK, BLOCK).astype(BF16))
            yield None
        total = jnp.sum(total, axis=0, keepdims=True)
        so[a, t] = (acc * (1.0 / total)).astype(BF16)
        sl[a, t] = top[0:1] + jnp.log2(total)
        yield None

    def o_copies(a, t):
        axis, here = AXES[1 - a], place[1 - a]
        away = (NR // 2 - lax.div(t + 1, 2)) * (1 - 2 * lax.rem(t + 1, 2))
        to = lax.rem(here + away + NR, NR)
        return (
            remote(so.at[a, t], ro.at[a, t], o_send.at[a, t], o_recv.at[a, t], axis, to),
            remote(sl.at[a, t], rl.at[a, t], l_send.at[a, t], l_recv.at[a, t], axis, to),
        )

    def run(generators):
        last = [None] * len(generators)
        alive = list(range(len(generators)))
        while alive:
            for g in list(alive):
                try:
                    value = next(generators[g])
                    if value is not None:
                        last[g] = value
                except StopIteration:
                    alive.remove(g)
        return last

    def attend(t, carry):
        (found0,) = run([first_pass(0, t)])
        _, found1 = run([second_pass(0, t, *found0), first_pass(1, t)])
        run([second_pass(1, t, *found1)])

        @pl.when(t < own)
        def _():
            for a in range(2):
                for copy in o_copies(a, t):
                    copy.start()

        return carry

    lax.fori_loop(0, NR, attend, 0)

    for a in range(2):
        for step in range(4):
            for copy in rings[a][step]:
                copy.wait_send()

    outs = []
    for a in range(2):
        for t in range(own):
            for copy in o_copies(a, t):
                copy.wait()
        logs = [rl[a, t] for t in range(own)] + [sl[a, own]]
        top = logs[0]
        for value in logs[1:]:
            top = jnp.maximum(top, value)
        total = None
        merged = None
        for t in range(NR):
            weight = jnp.exp2(logs[t] - top)
            block = so[a, own] if t == own else ro[a, t]
            term = block.astype(F32) * weight
            total = weight if total is None else total + weight
            merged = term if merged is None else merged + term
        outs.append(merged * (1.0 / total))
    mixed = outs[0] - lambdas[0] * outs[1]
    mixed = mixed * lax.rsqrt(jnp.mean(mixed * mixed, axis=0, keepdims=True) + EPSILON)
    attended = (jnp.transpose(mixed) * (hgain_v[...] * OUT_SCALE)).astype(BF16)
    for b in range(NX):
        att[b] = attended[b * ROWS : (b + 1) * ROWS]
    attr[x] = att[x]
    fifth = []
    for d in range(1, NX):
        to = lax.rem(x + d, NX)
        fifth.append(remote(att.at[to], attr.at[x], a_send.at[d], a_recv.at[d], "tp", to))
    for copy in fifth:
        copy.start()
    ow_relay_right.wait()
    ow_relay_left.wait()
    for copy in fifth:
        copy.wait()

    joined = jnp.concatenate([attr[b] for b in range(NX)], axis=1)
    gate = modulation(0, 2 * D)
    width = 512
    for c in range(D // width):
        lanes = slice(c * width, (c + 1) * width)
        weights = jnp.concatenate([ow[b, :, lanes] for b in range(NX)], axis=0)
        branch = dot(joined, weights)
        res[:, lanes] = (lat[x, :, lanes].astype(F32) + gate[:, lanes] * branch).astype(BF16)
    done = pltpu.make_async_copy(res, out.at[0], local_sem.at[9])
    done.start()
    done.wait()


def body(
    latent,
    condition,
    context,
    context_vector,
    modulator,
    norm_gain,
    query_weight,
    key_weight,
    value_weight,
    head_gain,
    lambdas,
    context_bias,
    out_weight,
):
    anywhere = pl.BlockSpec(memory_space=pl.ANY)
    vmem = pl.BlockSpec(memory_space=pltpu.VMEM)
    smem = pl.BlockSpec(memory_space=pltpu.SMEM)
    dma = pltpu.SemaphoreType.DMA
    return pl.pallas_call(
        kernel,
        out_shape=jax.ShapeDtypeStruct(latent.shape, latent.dtype),
        in_specs=[
            anywhere,
            vmem,
            anywhere,
            vmem,
            anywhere,
            anywhere,
            anywhere,
            anywhere,
            anywhere,
            anywhere,
            smem,
            smem,
            anywhere,
        ],
        out_specs=anywhere,
        scratch_shapes=[
            pltpu.VMEM((8, 3 * D), BF16),
            pltpu.VMEM((NX, 2, CHUNK), F32),
            pltpu.VMEM((NX, 2, CHUNK), F32),
            pltpu.VMEM((NR, 2, CHUNK), F32),
            pltpu.VMEM((NR, 2, CHUNK), F32),
            pltpu.VMEM((NX, 2, CHUNK), F32),
            pltpu.VMEM((NX, ROWS, D), BF16),
            pltpu.VMEM((CTX, D), BF16),
            pltpu.VMEM((1, D), F32),
            pltpu.VMEM((1, VAL), F32),
            pltpu.VMEM((D, 3 * VAL), BF16),
            pltpu.VMEM((NX, VAL, D), BF16),
            pltpu.VMEM((TALL, D), F32),
            pltpu.VMEM((TALL, D), BF16),
            pltpu.VMEM((2, NR, TALL, VAL), BF16),
            pltpu.VMEM((2, NR, VAL, BLOCK), BF16),
            pltpu.VMEM((2, NR * CTX, VAL), BF16),
            pltpu.VMEM((2, VAL, NR * CTX), BF16),
            pltpu.VMEM((2, NR * BLOCK, BLOCK), F32),
            pltpu.VMEM((2, NR, VAL, BLOCK), BF16),
            pltpu.VMEM((2, NR, 1, BLOCK), F32),
            pltpu.VMEM((2, NR, VAL, BLOCK), BF16),
            pltpu.VMEM((2, NR, 1, BLOCK), F32),
            pltpu.VMEM((NX, ROWS, VAL), BF16),
            pltpu.VMEM((NX, ROWS, VAL), BF16),
            pltpu.VMEM((ROWS, D), BF16),
            dma((10,)),
            dma((32,)),
            dma((32,)),
            dma((4,)),
            dma((4,)),
            dma((4,)),
            dma((4,)),
            dma((32,)),
            dma((32,)),
            dma((2, NR)),
            dma((2, NR)),
            dma((2, NR)),
            dma((2, NR)),
            dma((4,)),
            dma((4,)),
        ],
        compiler_params=pltpu.CompilerParams(
            collective_id=0, has_side_effects=True, vmem_limit_bytes=60 * 1024 * 1024
        ),
    )(
        latent,
        condition,
        context,
        context_vector.reshape(1, -1),
        modulator,
        norm_gain.reshape(1, -1),
        query_weight,
        key_weight,
        value_weight,
        head_gain.reshape(1, -1),
        lambdas,
        context_bias,
        out_weight,
    )


def solution(mesh):
    torus = Mesh(
        mesh.devices.reshape(8, 8, mesh.shape["tp"], mesh.shape["dp"]), ("sp_0", "sp_1", "tp", "dp")
    )
    return jax.shard_map(
        body,
        mesh=torus,
        in_specs=(
            P("dp", SP_TP, None),
            P("dp", SP_TP),
            P("dp", SP, None),
            P(SP_TP),
            P(SP_TP, None),
            P(),
            P(None, "tp"),
            P(None, "tp"),
            P(None, "tp"),
            P(),
            P("tp"),
            P("tp", None),
            P("tp", None),
        ),
        out_specs=P("dp", SP_TP, None),
        check_vma=False,
    )
```
